32 devices in a mesh: grp: 2 (over x), st: 4 (over y, core), tp: 4 (over z).
Axes of the slice: x: 2, y: 2, z: 4, core: 2. Of those that a mesh axis runs over, the one named last changes fastest.
Arguments:
- tokens: bfloat16 [2048, 2048], P(('grp', 'st')), parts along dimension 0, may hold values from -6 to 6
- pre_gain: float32 [2048], replicated, may hold values from 0.1 to 1.9
- w_gated: bfloat16 [2048, 1536], P(None, 'tp'), may hold values from -0.125 to 0.125
- w_mixed: bfloat16 [2048, 1536], P(None, 'tp'), may hold values from -0.125 to 0.125
- mix_weight: bfloat16 [8, 128, 128], P('tp'), may hold values from -0.5 to 0.5
- w_query: bfloat16 [2048, 1024], P(None, 'tp'), may hold values from -0.125 to 0.125
- w_gate_mix: bfloat16 [2048, 1536], P(None, 'tp'), may hold values from -0.125 to 0.125
- w_gate_read: bfloat16 [2048, 1024], P(None, 'tp'), may hold values from -0.125 to 0.125
- store: bfloat16 [64, 128, 2048], P(('grp', 'st')), parts along dimension 0, may hold values from -6 to 6
- mem_gain: float32 [2048], replicated, may hold values from 1 to 80
- w_key: bfloat16 [2048, 1024], P(None, 'tp'), may hold values from -0.125 to 0.125
- w_value: bfloat16 [2048, 1024], P(None, 'tp'), may hold values from -0.125 to 0.125
- passage_ids: int32 [32, 4], P(('grp', 'st')), parts along dimension 0, may hold values from 0 to 31, as said below
- w_out_mix: bfloat16 [1536, 2048], P('tp'), may hold values from -0.125 to 0.125
- w_out_read: bfloat16 [1024, 2048], P('tp'), may hold values from -0.125 to 0.125
Outputs:
- mixed_out: bfloat16 [2048, 2048], P(('grp', 'st', 'tp')), parts along dimension 0
The draws below stay inside these ranges and needn't reach their ends.
There are 2 independent parts, one for each index of `grp`. The reference program is written for one: setup_inputs(seed, part) draws one part's arguments, and reference() takes and returns one part's arrays. A program takes and returns all parts, laid end to end along the dimension named above; an argument that names none is the same for every part. Nothing has to cross between parts.
Inputs may be any that keep to these rules, and one draw needn't show every extreme that they name: `passage_ids`: passage p is held by index p // 8 of st. The 16 entries of one index of st name at most 8 passages held by any one index of st, and that most is reached in every draw.
All inputs are finite; a program needn't handle non-finite values.
Results may differ from the reference program's by a relative error of at most 0.015.
The reference program's roundings to bfloat16 on the way count: a program that leaves them out, or rounds other values in their place, can miss the bound.
Values may be sent and summed in bfloat16 or wider, within the bound.
A program may use at most 128 MiB of HBM per device.

```python
import jax
import jax.numpy as jnp
from jax import lax

D = 2048
GROUPS = 8
GW = 192
SW = 1536
XH = 8
HD = 128
XW = 1024
SPAN = 128
RBLOCK = 64
NPB = 4
PROWS = 128
PASS_DEV = 8
TOKENS = 1024
PASSAGES = 32
BLOCKS = 16
REQ = 16
CAP = 8
N_TP = 4


def draw_mem_gain(key, part):
    low_end = 1.0
    high_end = 4.0
    unit = jax.random.uniform(key, (D,), jnp.float32)
    return jnp.exp(jnp.log(low_end) + unit * (jnp.log(high_end) - jnp.log(low_end)))


def draw_passage_ids(key, part):
    readers = PASSAGES // PASS_DEV
    key_pop, key_rest = jax.random.split(jax.random.fold_in(key, 17))
    popular = jax.random.randint(key_pop, (readers,), 0, 4)
    slot_count = readers * CAP
    slot_owner = jnp.arange(slot_count, dtype=jnp.int32) // CAP
    slot_copy = jnp.arange(slot_count, dtype=jnp.int32) % CAP

    def one_reader(reader, reader_key):
        key_noise, key_left, key_right, key_order = jax.random.split(reader_key, 4)
        noise = jax.random.randint(key_noise, (slot_count,), 0, 64)
        score = popular[slot_owner] * 64 + noise
        before = slot_owner == (reader + readers - 1) % readers
        across = (slot_owner == (reader + readers // 2) % readers) & (slot_copy == 0)
        score = jnp.where(before | across, 100000, score)
        score = score * 4096 + jnp.arange(slot_count, dtype=jnp.int32)
        ranking = jnp.argsort(-score, stable=True)
        chosen = slot_owner[ranking[:REQ]]
        within = jnp.minimum(jax.random.randint(key_left, (REQ,), 0, PASS_DEV), jax.random.randint(key_right, (REQ,), 0, PASS_DEV))
        picked = (chosen * PASS_DEV + within).astype(jnp.int32)
        return picked[jax.random.permutation(key_order, REQ)]
    reader_keys = jax.random.split(key_rest, readers)
    every = jax.vmap(one_reader)(jnp.arange(readers, dtype=jnp.int32), reader_keys)
    return every.reshape(BLOCKS, NPB).astype(jnp.int32)


def block_levels(rng, shape, cuts, low, top_value):
    def one(position, parts):
        draws = jax.random.uniform(jax.random.fold_in(jax.random.fold_in(rng, 6), position), (parts,), jnp.float32, low / len(cuts), top_value / len(cuts))
        return jnp.repeat(jnp.exp(draws), shape[position] // parts).reshape((-1,) + (1,) * (len(shape) - position - 1))

    loudness = one(*cuts[0])
    for cut in cuts[1:]:
        loudness = loudness * one(*cut)
    return loudness


def gaussian(key, extent, scale, bound, pieces=(), held_as=jnp.bfloat16):
    result = scale * jax.random.normal(key, extent, jnp.float32)
    if pieces:
        result = result * block_levels(key, extent, pieces, -0.22, 0.18)
    return jnp.clip(result, -bound, bound).astype(held_as)


def setup_inputs(seed: int = 0, part: int = 0) -> dict:
    key_list = jax.random.split(jax.random.key(seed), 16)
    part_keys = jax.random.split(jax.random.fold_in(key_list[15], part), 16)
    tokens = gaussian(part_keys[0], (TOKENS, D), 1.0, 6.0, ((0, 4),))
    pre_gain = jnp.clip(1.0 + 0.18 * jax.random.normal(key_list[1], (D,), jnp.float32), 0.1, 1.9)
    w_gated = gaussian(key_list[2], (D, SW), D ** -0.5, 0.125, ((1, 4),))
    w_mixed = gaussian(key_list[3], (D, SW), D ** -0.5, 0.125, ((1, 4),))
    mix_weight = gaussian(key_list[4], (GROUPS, SPAN, SPAN), SPAN ** -0.5, 0.5, ((0, 4),))
    w_query = gaussian(key_list[5], (D, XW), D ** -0.5, 0.125, ((1, 4),))
    w_gate_mix = gaussian(key_list[6], (D, SW), D ** -0.5, 0.125, ((1, 4),))
    w_gate_read = gaussian(key_list[7], (D, XW), D ** -0.5, 0.125, ((1, 4),))
    store = gaussian(part_keys[8], (PASSAGES, PROWS, D), 1.0, 6.0, ((0, 4),))
    mem_gain = draw_mem_gain(jax.random.fold_in(key_list[15], 71), part)
    w_key = gaussian(key_list[10], (D, XW), D ** -0.5, 0.125, ((1, 4),))
    w_value = gaussian(key_list[11], (D, XW), D ** -0.5, 0.125, ((1, 4),))
    passage_ids = draw_passage_ids(jax.random.fold_in(jax.random.fold_in(key_list[15], part), 71), part)
    w_out_mix = gaussian(key_list[13], (SW, D), (SW + XW) ** -0.5, 0.125, ((0, 4),))
    w_out_read = gaussian(key_list[14], (XW, D), (SW + XW) ** -0.5, 0.125, ((0, 4),))
    return dict(tokens=tokens, pre_gain=pre_gain, w_gated=w_gated, w_mixed=w_mixed, mix_weight=mix_weight, w_query=w_query, w_gate_mix=w_gate_mix, w_gate_read=w_gate_read, store=store, mem_gain=mem_gain, w_key=w_key, w_value=w_value, passage_ids=passage_ids, w_out_mix=w_out_mix, w_out_read=w_out_read)


eps = 1e-06

def reference(tokens, pre_gain, w_gated, w_mixed, mix_weight, w_query, w_gate_mix, w_gate_read, store, mem_gain, w_key, w_value, passage_ids, w_out_mix, w_out_read):
    inputs = tokens.astype(jnp.float32)
    normed = (inputs * lax.rsqrt(lax.optimization_barrier(jnp.mean(inputs * inputs, axis=-1, keepdims=True)) + eps) * pre_gain).astype(jnp.bfloat16)
    gated = jnp.dot(normed, w_gated, preferred_element_type=jnp.float32)
    mixed_in = jnp.dot(normed, w_mixed, preferred_element_type=jnp.float32)
    grouped = mixed_in.reshape(TOKENS, GROUPS, GW)
    group_mean = lax.optimization_barrier(jnp.mean(grouped, axis=-1, keepdims=True))
    centred = grouped - group_mean
    group_var = lax.optimization_barrier(jnp.mean(centred * centred, axis=-1, keepdims=True))
    mixed_norm = (centred * lax.rsqrt(group_var + eps)).astype(jnp.bfloat16)
    causal = jnp.tril(jnp.ones((SPAN, SPAN), dtype=bool))
    mix_masked = jnp.where(causal[None], mix_weight.astype(jnp.float32), 0.0)
    blocked = mixed_norm.reshape(TOKENS // SPAN, SPAN, GROUPS, GW).astype(jnp.float32)
    spatial = jnp.einsum('hts,nshd->nthd', mix_masked, blocked).reshape(TOKENS, SW)
    branch_mix = gated * spatial
    query = jnp.dot(normed, w_query, preferred_element_type=jnp.float32).astype(jnp.bfloat16)
    read_rows = store[passage_ids.reshape(-1)].astype(jnp.float32)
    passage_norm = (read_rows * lax.rsqrt(lax.optimization_barrier(jnp.mean(read_rows * read_rows, axis=-1, keepdims=True)) + eps) * mem_gain).astype(jnp.bfloat16)
    flat_rows = passage_norm.reshape(-1, D)
    keys = jnp.dot(flat_rows, w_key, preferred_element_type=jnp.float32).astype(jnp.bfloat16).reshape(BLOCKS, NPB * PROWS, XH, HD)
    values = jnp.dot(flat_rows, w_value, preferred_element_type=jnp.float32).astype(jnp.bfloat16).reshape(BLOCKS, NPB * PROWS, XH, HD)
    query_blocks = query.reshape(BLOCKS, RBLOCK, XH, HD).astype(jnp.float32)
    scores = jnp.einsum('btha,bkha->bhtk', query_blocks, keys.astype(jnp.float32)) * HD ** (-0.5)
    probs = jax.nn.softmax(scores, axis=-1).astype(jnp.bfloat16)
    branch_read = jnp.einsum('bhtk,bkha->btha', probs.astype(jnp.float32), values.astype(jnp.float32)).reshape(TOKENS, XW)
    gate_mix = jnp.dot(normed, w_gate_mix, preferred_element_type=jnp.float32)
    gate_read = jnp.dot(normed, w_gate_read, preferred_element_type=jnp.float32)
    out_mix = (branch_mix * jax.nn.silu(gate_mix)).astype(jnp.bfloat16)
    out_read = (branch_read * jax.nn.silu(gate_read)).astype(jnp.bfloat16)
    mix_cols = SW // N_TP
    read_cols = XW // N_TP
    total = jnp.zeros((TOKENS, D), jnp.float32)
    for shard in range(N_TP):
        partial_value = jnp.dot(out_mix[:, shard * mix_cols:(shard + 1) * mix_cols], w_out_mix[shard * mix_cols:(shard + 1) * mix_cols], preferred_element_type=jnp.float32)
        partial_value = partial_value + jnp.dot(out_read[:, shard * read_cols:(shard + 1) * read_cols], w_out_read[shard * read_cols:(shard + 1) * read_cols], preferred_element_type=jnp.float32)
        total = total + lax.optimization_barrier(partial_value.astype(jnp.bfloat16)).astype(jnp.float32)
    return total.astype(jnp.bfloat16)
```

```python
import functools

import jax
import jax.numpy as jnp
from jax import lax
from jax.experimental import pallas as pl
from jax.experimental.pallas import tpu as pltpu
from jax.sharding import PartitionSpec as P

HD = 128
SPAN = 128
RBLOCK = 64
EPS = 1e-06
LOG2E = 1.4426950408889634
SUBS = 2
BF = jnp.bfloat16
F32 = jnp.float32
MESH = pl.DeviceIdType.MESH


def rms_rows(rows, gain):
    wide = rows.astype(F32)
    return (wide * lax.rsqrt(jnp.mean(wide * wide, axis=-1, keepdims=True) + EPS) * gain).astype(BF)


def silu(v):
    return v / (1.0 + jnp.exp(-v))


def dot(a, b):
    return jnp.dot(a, b, preferred_element_type=F32)


def kernel(
    n_st, n_tp,
    tok_h, pg_h, wga_h, wmi_h, mw_h, wq_h, wgm_h, wgr_h, sto_h, mg_h, wk_h, wv_h, pid, wom_h, wor_h,
    out_ref,
    tok, pg, wga, wmi, mw, wq, wgm, wgr, sto, mg, wk, wv, wom, wor,
    normed, q_buf, c_send, c_buf, k_s, vt_s, s_s, p_s, o_send, o_buf, t_send, t_buf,
    om, orr, r_send, r_buf,
    in_sem, q_ss, q_rs, c_ss, c_rs, o_ss, o_rs, t_ss, t_rs, r_ss, r_rs,
):
    st = lax.axis_index("st")
    tp = lax.axis_index("tp")
    rows = tok.shape[0]
    held = sto.shape[0]
    prow = sto.shape[1]
    width = wq.shape[1]
    heads = width // HD
    groups = mw.shape[0]
    gw = wmi.shape[1] // groups
    scale = (HD ** -0.5) * LOG2E

    pieces = sto_step = 4 if held % 4 == 0 else 1
    per = held // pieces
    loads = {}
    order = [("tok", tok_h, tok), ("pg", pg_h, pg), ("wq", wq_h, wq), ("mg", mg_h, mg),
             ("wk", wk_h, wk), ("wv", wv_h, wv)]
    late = [("wmi", wmi_h, wmi), ("wga", wga_h, wga), ("wgm", wgm_h, wgm), ("wgr", wgr_h, wgr),
            ("mw", mw_h, mw), ("wom", wom_h, wom), ("wor", wor_h, wor)]
    for i, (name, src, dst) in enumerate(order):
        loads[name] = pltpu.make_async_copy(src, dst, in_sem.at[i])
        loads[name].start()
    base = len(order)

    def store_copy(i):
        return pltpu.make_async_copy(
            sto_h.at[pl.ds(i * per, per)], sto.at[pl.ds(i * per, per)], in_sem.at[base + i]
        )

    for i in range(pieces):
        store_copy(i).start()
    for i, (name, src, dst) in enumerate(late):
        loads[name] = pltpu.make_async_copy(src, dst, in_sem.at[base + pieces + i])
        loads[name].start()

    barrier = pltpu.get_barrier_semaphore()
    for off in range(1, n_st):
        pl.semaphore_signal(barrier, inc=1, device_id={"st": lax.rem(st + off, n_st)}, device_id_type=MESH)
    right = lax.rem(tp + 1, n_tp)
    left = lax.rem(tp + n_tp - 1, n_tp)
    for side in (left, right):
        pl.semaphore_signal(barrier, inc=1, device_id={"tp": side}, device_id_type=MESH)

    lane_block = lax.broadcasted_iota(jnp.int32, (held, rows), 1) // RBLOCK
    row_id = lax.broadcasted_iota(jnp.int32, (held, rows), 0)
    for off in range(n_st):
        mine = row_id + lax.rem(st + off, n_st) * held
        count = jnp.zeros((held, rows), F32)
        for b in range(pid.shape[0]):
            hit = jnp.zeros((held, rows), F32)
            for n in range(pid.shape[1]):
                hit = hit + jnp.where(mine == pid[b, n], 1.0, 0.0)
            count = count + jnp.where(lane_block == b, hit, 0.0)
        c_send[off] = count

    loads["tok"].wait()
    loads["pg"].wait()
    chunk = 64
    gain = pg[...]

    def norm_step(i, carry):
        at = pl.ds(pl.multiple_of(i * chunk, chunk), chunk)
        normed[at, :] = rms_rows(tok[at, :], gain)
        return carry

    lax.fori_loop(0, rows // chunk, norm_step, 0)
    loads["wq"].wait()
    q_buf[0] = dot(normed[...], wq[...]).astype(BF)

    pl.semaphore_wait(barrier, n_st + 1)

    def remote(src, dst, ss, rs, axis, to):
        return pltpu.make_async_remote_copy(
            src_ref=src, dst_ref=dst, send_sem=ss, recv_sem=rs, device_id={axis: to}, device_id_type=MESH
        )

    q_cp, c_cp, o_cp, t_cp = {}, {}, {}, {}
    for off in range(1, n_st):
        to = lax.rem(st + off, n_st)
        c_cp[off] = remote(c_send.at[off], c_buf.at[off], c_ss.at[off], c_rs.at[off], "st", to)
        q_cp[off] = remote(q_buf.at[0], q_buf.at[off], q_ss.at[off], q_rs.at[off], "st", to)
        c_cp[off].start()
        q_cp[off].start()
    c_buf[0] = c_send[0]

    loads["mg"].wait()
    loads["wk"].wait()
    loads["wv"].wait()
    mgain = mg[...]
    span = per * prow

    def kv_step(i, carry):
        store_copy(i).wait()
        part = sto[pl.ds(i * per, per)].reshape(span, sto.shape[2])
        rows_n = rms_rows(part, mgain)
        at = pl.ds(pl.multiple_of(i * span, span), span)
        k_s[at, :] = dot(rows_n, wk[...]).astype(BF)
        vt_s[:, at] = dot(rows_n, wv[...]).T.astype(BF)
        return carry

    lax.fori_loop(0, pieces, kv_step, 0)

    loads["wmi"].wait()
    mixed = dot(normed[...], wmi[...])
    gid = lax.broadcasted_iota(jnp.int32, (1, mixed.shape[1]), 1) // gw
    centre = mixed
    for g in range(groups):
        mean = jnp.sum(jnp.where(gid == g, mixed, 0.0), axis=-1, keepdims=True) * (1.0 / gw)
        centre = jnp.where(gid == g, mixed - mean, centre)
    square = centre * centre
    factor = jnp.zeros_like(mixed)
    for g in range(groups):
        var = jnp.sum(jnp.where(gid == g, square, 0.0), axis=-1, keepdims=True) * (1.0 / gw)
        factor = jnp.where(gid == g, lax.rsqrt(var + EPS), factor)
    mixed_norm = (centre * factor).astype(BF)

    def attend(off):
        reader_counts = c_buf[off]
        stats = []
        for h in range(heads):
            cols = slice(h * HD, (h + 1) * HD)
            s_s[...] = lax.dot_general(
                k_s[:, cols], q_buf[off, :, cols], (((1,), (1,)), ((), ())), preferred_element_type=F32
            )
            top = jnp.full((1, rows), -1e30, F32)
            for j in range(held):
                one = jnp.max(s_s[j * prow:(j + 1) * prow, :], axis=0, keepdims=True)
                top = jnp.where(reader_counts[j:j + 1, :] > 0.0, jnp.maximum(top, one), top)
            total = jnp.zeros((1, rows), F32)
            for j in range(held):
                at = slice(j * prow, (j + 1) * prow)
                times = reader_counts[j:j + 1, :]
                off_by = jnp.where(times > 0.0, top, 1e30)
                e = jnp.exp2((s_s[at, :] - off_by) * scale) * times
                total = total + jnp.sum(e, axis=0, keepdims=True)
                p_s[at, :] = e.astype(BF)
            inverse = jnp.where(total > 0.0, 1.0 / jnp.where(total > 0.0, total, 1.0), 0.0)
            read = dot(vt_s[cols, :], p_s[...]) * inverse
            if off == 0:
                o_buf[0, cols, :] = read.astype(BF)
            else:
                o_send[off, cols, :] = read.astype(BF)
            stats += [top, total]
        pad = t_send.shape[1] - len(stats)
        if pad:
            stats.append(jnp.zeros((pad, rows), F32))
        if off == 0:
            t_buf[0] = jnp.concatenate(stats, axis=0)
        else:
            t_send[off] = jnp.concatenate(stats, axis=0)

    for off in range(1, n_st):
        c_cp[off].wait_recv()
        q_cp[off].wait_recv()
        attend(off)
        to = lax.rem(st + n_st - off, n_st)
        t_cp[off] = remote(t_send.at[off], t_buf.at[off], t_ss.at[off], t_rs.at[off], "st", to)
        o_cp[off] = remote(o_send.at[off], o_buf.at[off], o_ss.at[off], o_rs.at[off], "st", to)
        t_cp[off].start()
        o_cp[off].start()
    attend(0)

    loads["mw"].wait()
    lower = lax.broadcasted_iota(jnp.int32, (SPAN, SPAN), 1) <= lax.broadcasted_iota(jnp.int32, (SPAN, SPAN), 0)
    weights = [jnp.where(lower, mw[g].astype(F32), 0.0).astype(BF) for g in range(groups)]
    parts = []
    for n in range(rows // SPAN):
        block = mixed_norm[n * SPAN:(n + 1) * SPAN, :]
        spatial = dot(weights[0], block)
        for g in range(1, groups):
            spatial = jnp.where(gid == g, dot(weights[g], block), spatial)
        parts.append(spatial)
    spatial = jnp.concatenate(parts, axis=0)
    loads["wga"].wait()
    branch = dot(normed[...], wga[...]) * spatial
    loads["wgm"].wait()
    om[...] = (branch * silu(dot(normed[...], wgm[...]))).astype(BF)
    loads["wgr"].wait()
    gate_read = silu(dot(normed[...], wgr[...]))

    for off in range(1, n_st):
        t_cp[off].wait_recv()
        o_cp[off].wait_recv()
    for h in range(heads):
        cols = slice(h * HD, (h + 1) * HD)
        tops = [t_buf[i, 2 * h:2 * h + 1, :] for i in range(n_st)]
        top = functools.reduce(jnp.maximum, tops)
        shares = [jnp.exp2((tops[i] - top) * scale) * t_buf[i, 2 * h + 1:2 * h + 2, :] for i in range(n_st)]
        inverse = 1.0 / functools.reduce(jnp.add, shares)
        read = jnp.zeros((HD, rows), F32)
        for i in range(n_st):
            read = read + o_buf[i, cols, :].astype(F32) * (shares[i] * inverse)
        orr[:, cols] = (read.T * gate_read[:, cols]).astype(BF)

    loads["wom"].wait()
    loads["wor"].wait()
    take = rows // n_tp
    piece = wom.shape[1] // (2 * SUBS)

    def partial(index, chain):
        at = pl.ds(pl.multiple_of(index * take, take), take)
        cols = slice(chain * piece, (chain + 1) * piece)
        return dot(om[at, :], wom[:, cols]) + dot(orr[at, :], wor[:, cols])

    r_cp = {}

    def ring(chain, step):
        return remote(
            r_send.at[step, chain], r_buf.at[step, chain], r_ss.at[step, chain], r_rs.at[step, chain],
            "tp", right if chain % 2 == 0 else left,
        )

    for step in range(n_tp):
        for chain in range(2 * SUBS):
            if chain % 2 == 0:
                index = lax.rem(tp + 2 * n_tp - 1 - step, n_tp)
            else:
                index = lax.rem(tp + 1 + step, n_tp)
            value = partial(index, chain)
            if step:
                r_cp[step - 1, chain].wait_recv()
                value = value + r_buf[step - 1, chain].astype(F32)
            if step < n_tp - 1:
                r_send[step, chain] = value.astype(BF)
                r_cp[step, chain] = ring(chain, step)
                r_cp[step, chain].start()
            else:
                out_ref[:, chain * piece:(chain + 1) * piece] = value.astype(BF)

    for off in range(1, n_st):
        for cp in (c_cp, q_cp, t_cp, o_cp):
            cp[off].wait_send()
    for cp in r_cp.values():
        cp.wait_send()


def local(
    tokens, pre_gain, w_gated, w_mixed, mix_weight, w_query, w_gate_mix, w_gate_read,
    store, mem_gain, w_key, w_value, passage_ids, w_out_mix, w_out_read,
):
    n_st = lax.axis_size("st")
    n_tp = lax.axis_size("tp")
    args = [
        tokens, pre_gain.reshape(1, -1), w_gated, w_mixed, mix_weight, w_query, w_gate_mix, w_gate_read,
        store, mem_gain.reshape(1, -1), w_key, w_value, passage_ids, w_out_mix, w_out_read,
    ]
    rows, model = tokens.shape
    width = w_query.shape[1]
    held, prow = store.shape[:2]
    stat_rows = max(8, 2 * (width // HD))
    take = rows // n_tp
    piece = model // (2 * SUBS)
    anyspace = pl.BlockSpec(memory_space=pl.ANY)
    specs = [anyspace] * len(args)
    specs[12] = pl.BlockSpec(memory_space=pltpu.SMEM)
    vm = pltpu.VMEM
    dma = pltpu.SemaphoreType.DMA
    scratch = [vm(a.shape, a.dtype) for i, a in enumerate(args) if i != 12]
    scratch += [
        vm((rows, model), BF),
        vm((n_st, rows, width), BF),
        vm((n_st, held, rows), F32),
        vm((n_st, held, rows), F32),
        vm((held * prow, width), BF),
        vm((width, held * prow), BF),
        vm((held * prow, rows), F32),
        vm((held * prow, rows), BF),
        vm((n_st, width, rows), BF),
        vm((n_st, width, rows), BF),
        vm((n_st, stat_rows, rows), F32),
        vm((n_st, stat_rows, rows), F32),
        vm((rows, w_gated.shape[1]), BF),
        vm((rows, width), BF),
        vm((n_tp - 1, 2 * SUBS, take, piece), BF),
        vm((n_tp - 1, 2 * SUBS, take, piece), BF),
        dma((24,)),
    ]
    scratch += [dma((n_st,))] * 8 + [dma((n_tp - 1, 2 * SUBS))] * 2
    return pl.pallas_call(
        functools.partial(kernel, n_st, n_tp),
        out_shape=jax.ShapeDtypeStruct((take, model), BF),
        in_specs=specs,
        out_specs=pl.BlockSpec(memory_space=pltpu.VMEM),
        scratch_shapes=scratch,
        compiler_params=pltpu.CompilerParams(
            collective_id=0, has_side_effects=True, vmem_limit_bytes=60 * 1024 * 1024
        ),
    )(*args)


def solution(mesh):
    placed = (
        P(("grp", "st"), None),
        P(),
        P(None, "tp"),
        P(None, "tp"),
        P("tp", None, None),
        P(None, "tp"),
        P(None, "tp"),
        P(None, "tp"),
        P(("grp", "st"), None, None),
        P(),
        P(None, "tp"),
        P(None, "tp"),
        P(("grp", "st"), None),
        P("tp", None),
        P("tp", None),
    )
    return jax.shard_map(
        local, mesh=mesh, in_specs=placed, out_specs=P(("grp", "st", "tp"), None), check_vma=False
    )
```

```python
import functools

import jax
import jax.numpy as jnp
from jax import lax
from jax.experimental import pallas as pl
from jax.experimental.pallas import tpu as pltpu
from jax.sharding import PartitionSpec as P

HD = 128
SPAN = 128
RBLOCK = 64
EPS = 1e-06
LOG2E = 1.4426950408889634
SUBS = 2
BF = jnp.bfloat16
F32 = jnp.float32
MESH = pl.DeviceIdType.MESH


def rms_rows(rows, gain):
    wide = rows.astype(F32)
    return (wide * lax.rsqrt(jnp.mean(wide * wide, axis=-1, keepdims=True) + EPS) * gain).astype(BF)


def silu(v):
    return v / (1.0 + jnp.exp(-v))


def dot(a, b):
    return jnp.dot(a, b, preferred_element_type=F32)


def kernel(
    n_st, n_tp,
    tok_h, pg_h, wga_h, wmi_h, mw_h, wq_h, wgm_h, wgr_h, sto_h, mg_h, wk_h, wv_h, pid_h, wom_h, wor_h,
    out_ref,
    tok, pg, wga, wmi, mw, wq, wgm, wgr, sto, mg, wk, wv, wom, wor,
    normed, q_buf, c_send, c_buf, k_s, vt_s, s_s, p_s, o_send, o_buf, t_send, t_buf,
    om, orr, r_send, r_buf, own, pid,
    in_sem, q_ss, q_rs, c_ss, c_rs, o_ss, o_rs, t_ss, t_rs, r_ss, r_rs,
):
    st = lax.axis_index("st")
    tp = lax.axis_index("tp")
    rows = tok.shape[0]
    held = sto.shape[0]
    prow = sto.shape[1]
    width = wq.shape[1]
    heads = width // HD
    groups = mw.shape[0]
    gw = wmi.shape[1] // groups
    scale = (HD ** -0.5) * LOG2E

    pieces = 4 if held % 4 == 0 else 1
    per = held // pieces
    loads = {}
    order = [("pid", pid_h, pid), ("tok", tok_h, tok), ("pg", pg_h, pg), ("wq", wq_h, wq), ("mg", mg_h, mg),
             ("wk", wk_h, wk), ("wv", wv_h, wv)]
    late = [("wmi", wmi_h, wmi), ("wga", wga_h, wga), ("wgm", wgm_h, wgm), ("wgr", wgr_h, wgr),
            ("mw", mw_h, mw), ("wom", wom_h, wom), ("wor", wor_h, wor)]
    for i, (name, src, dst) in enumerate(order):
        loads[name] = pltpu.make_async_copy(src, dst, in_sem.at[i])
        loads[name].start()
    base = len(order)

    def store_copy(i):
        return pltpu.make_async_copy(
            sto_h.at[pl.ds(i * per, per)], sto.at[pl.ds(i * per, per)], in_sem.at[base + i]
        )

    for i in range(pieces):
        store_copy(i).start()
    for i, (name, src, dst) in enumerate(late):
        loads[name] = pltpu.make_async_copy(src, dst, in_sem.at[base + pieces + i])
        loads[name].start()

    barrier = pltpu.get_barrier_semaphore()
    for off in range(1, n_st):
        pl.semaphore_signal(barrier, inc=1, device_id={"st": lax.rem(st + off, n_st)}, device_id_type=MESH)
    right = lax.rem(tp + 1, n_tp)
    left = lax.rem(tp + n_tp - 1, n_tp)
    for side in (left, right):
        pl.semaphore_signal(barrier, inc=1, device_id={"tp": side}, device_id_type=MESH)

    loads["tok"].wait()
    loads["pg"].wait()
    chunk = 64
    gain = pg[...]

    def norm_step(i, carry):
        at = pl.ds(pl.multiple_of(i * chunk, chunk), chunk)
        normed[at, :] = rms_rows(tok[at, :], gain)
        return carry

    lax.fori_loop(0, rows // chunk, norm_step, 0)
    loads["pid"].wait()
    lane_block = lax.broadcasted_iota(jnp.int32, (held, rows), 1) // RBLOCK
    row_id = lax.broadcasted_iota(jnp.int32, (held, rows), 0)
    for off in range(n_st):
        mine = row_id + lax.rem(st + off, n_st) * held
        count = jnp.zeros((held, rows), F32)
        for b in range(pid.shape[0]):
            hit = jnp.zeros((held, rows), F32)
            for n in range(pid.shape[1]):
                hit = hit + jnp.where(mine == pid[b, n], 1.0, 0.0)
            count = count + jnp.where(lane_block == b, hit, 0.0)
        c_send[off] = count
    loads["wq"].wait()
    q_buf[0] = dot(normed[...], wq[...]).astype(BF)

    pl.semaphore_wait(barrier, n_st + 1)

    def remote(src, dst, ss, rs, axis, to):
        return pltpu.make_async_remote_copy(
            src_ref=src, dst_ref=dst, send_sem=ss, recv_sem=rs, device_id={axis: to}, device_id_type=MESH
        )

    q_cp, c_cp, o_cp, t_cp = {}, {}, {}, {}
    for off in range(1, n_st):
        to = lax.rem(st + off, n_st)
        c_cp[off] = remote(c_send.at[off], c_buf.at[off], c_ss.at[off], c_rs.at[off], "st", to)
        q_cp[off] = remote(q_buf.at[0], q_buf.at[off], q_ss.at[off], q_rs.at[off], "st", to)
        c_cp[off].start()
        q_cp[off].start()
    c_buf[0] = c_send[0]

    loads["mg"].wait()
    loads["wk"].wait()
    loads["wv"].wait()
    mgain = mg[...]
    span = per * prow

    def kv_step(i, carry):
        store_copy(i).wait()
        part = sto[pl.ds(i * per, per)].reshape(span, sto.shape[2])
        rows_n = rms_rows(part, mgain)
        at = pl.ds(pl.multiple_of(i * span, span), span)
        k_s[at, :] = dot(rows_n, wk[...]).astype(BF)
        vt_s[:, at] = dot(rows_n, wv[...]).T.astype(BF)
        return carry

    lax.fori_loop(0, pieces, kv_step, 0)

    loads["wmi"].wait()
    mixed = dot(normed[...], wmi[...])
    gid = lax.broadcasted_iota(jnp.int32, (1, mixed.shape[1]), 1) // gw
    centre = mixed
    for g in range(groups):
        mean = jnp.sum(jnp.where(gid == g, mixed, 0.0), axis=-1, keepdims=True) * (1.0 / gw)
        centre = jnp.where(gid == g, mixed - mean, centre)
    square = centre * centre
    factor = jnp.zeros_like(mixed)
    for g in range(groups):
        var = jnp.sum(jnp.where(gid == g, square, 0.0), axis=-1, keepdims=True) * (1.0 / gw)
        factor = jnp.where(gid == g, lax.rsqrt(var + EPS), factor)
    mixed_norm = (centre * factor).astype(BF)

    def attend(off):
        reader_counts = c_buf[off]
        stats = []
        for h in range(heads):
            cols = slice(h * HD, (h + 1) * HD)
            s_s[...] = lax.dot_general(
                k_s[:, cols], q_buf[off, :, cols], (((1,), (1,)), ((), ())), preferred_element_type=F32
            )
            top = jnp.full((1, rows), -1e30, F32)
            for j in range(held):
                one = jnp.max(s_s[j * prow:(j + 1) * prow, :], axis=0, keepdims=True)
                top = jnp.where(reader_counts[j:j + 1, :] > 0.0, jnp.maximum(top, one), top)
            total = jnp.zeros((1, rows), F32)
            for j in range(held):
                at = slice(j * prow, (j + 1) * prow)
                times = reader_counts[j:j + 1, :]
                off_by = jnp.where(times > 0.0, top, 1e30)
                e = jnp.exp2((s_s[at, :] - off_by) * scale) * times
                total = total + jnp.sum(e, axis=0, keepdims=True)
                p_s[at, :] = e.astype(BF)
            inverse = jnp.where(total > 0.0, 1.0 / jnp.where(total > 0.0, total, 1.0), 0.0)
            read = dot(vt_s[cols, :], p_s[...]) * inverse
            if off == 0:
                o_buf[0, cols, :] = read.astype(BF)
            else:
                o_send[off, cols, :] = read.astype(BF)
            stats += [top, total]
        pad = t_send.shape[1] - len(stats)
        if pad:
            stats.append(jnp.zeros((pad, rows), F32))
        if off == 0:
            t_buf[0] = jnp.concatenate(stats, axis=0)
        else:
            t_send[off] = jnp.concatenate(stats, axis=0)

    for off in range(1, n_st):
        c_cp[off].wait_recv()
        q_cp[off].wait_recv()
        attend(off)
        to = lax.rem(st + n_st - off, n_st)
        t_cp[off] = remote(t_send.at[off], t_buf.at[off], t_ss.at[off], t_rs.at[off], "st", to)
        o_cp[off] = remote(o_send.at[off], o_buf.at[off], o_ss.at[off], o_rs.at[off], "st", to)
        t_cp[off].start()
        o_cp[off].start()
    attend(0)

    loads["mw"].wait()
    lower = lax.broadcasted_iota(jnp.int32, (SPAN, SPAN), 1) <= lax.broadcasted_iota(jnp.int32, (SPAN, SPAN), 0)
    weights = [jnp.where(lower, mw[g].astype(F32), 0.0).astype(BF) for g in range(groups)]
    parts = []
    for n in range(rows // SPAN):
        block = mixed_norm[n * SPAN:(n + 1) * SPAN, :]
        spatial = dot(weights[0], block)
        for g in range(1, groups):
            spatial = jnp.where(gid == g, dot(weights[g], block), spatial)
        parts.append(spatial)
    spatial = jnp.concatenate(parts, axis=0)
    loads["wga"].wait()
    branch = dot(normed[...], wga[...]) * spatial
    loads["wgm"].wait()
    om[...] = (branch * silu(dot(normed[...], wgm[...]))).astype(BF)
    loads["wgr"].wait()
    gate_read = silu(dot(normed[...], wgr[...]))

    for off in range(1, n_st):
        t_cp[off].wait_recv()
        o_cp[off].wait_recv()
    for h in range(heads):
        cols = slice(h * HD, (h + 1) * HD)
        tops = [t_buf[i, 2 * h:2 * h + 1, :] for i in range(n_st)]
        top = functools.reduce(jnp.maximum, tops)
        shares = [jnp.exp2((tops[i] - top) * scale) * t_buf[i, 2 * h + 1:2 * h + 2, :] for i in range(n_st)]
        inverse = 1.0 / functools.reduce(jnp.add, shares)
        read = jnp.zeros((HD, rows), F32)
        for i in range(n_st):
            read = read + o_buf[i, cols, :].astype(F32) * (shares[i] * inverse)
        orr[:, cols] = (read.T * gate_read[:, cols]).astype(BF)

    loads["wom"].wait()
    loads["wor"].wait()
    take = rows // n_tp
    piece = wom.shape[1] // SUBS

    def partial(index, chain):
        at = pl.ds(pl.multiple_of(index * take, take), take)
        cols = slice(chain * piece, (chain + 1) * piece)
        return dot(om[at, :], wom[:, cols]) + dot(orr[at, :], wor[:, cols])

    def hop(way, index, sub):
        return remote(
            r_send.at[way, index, sub], r_buf.at[way, index, sub],
            r_ss.at[way, index, sub], r_rs.at[way, index, sub],
            "tp", left if way else right,
        )

    def forward(way, index, sub):
        sends = tp > index if way else tp < index
        takes = tp < n_tp - 1 if way else tp > 0

        @pl.when(sends & takes)
        def _():
            value = partial(index, sub)
            hop(way, index, sub).wait_recv()
            r_send[way, index, sub] = (value + r_buf[way, index, sub].astype(F32)).astype(BF)
            hop(way, index, sub).start()

        @pl.when(sends & jnp.logical_not(takes))
        def _():
            r_send[way, index, sub] = partial(index, sub).astype(BF)
            hop(way, index, sub).start()

    for k in range(n_tp - 1):
        for sub in range(SUBS):
            forward(0, n_tp - 1 - k, sub)
            forward(1, k, sub)

    for sub in range(SUBS):
        own[:, sub * piece:(sub + 1) * piece] = partial(tp, sub)
    for index in range(n_tp):
        @pl.when(tp == index)
        def _():
            for sub in range(SUBS):
                value = own[:, sub * piece:(sub + 1) * piece]
                if index < n_tp - 1:
                    hop(1, index, sub).wait_recv()
                    value = value + r_buf[1, index, sub].astype(F32)
                if index > 0:
                    hop(0, index, sub).wait_recv()
                    value = value + r_buf[0, index, sub].astype(F32)
                out_ref[:, sub * piece:(sub + 1) * piece] = value.astype(BF)

    for k in range(n_tp - 1):
        for sub in range(SUBS):
            for way, index in ((0, n_tp - 1 - k), (1, k)):
                @pl.when(tp > index if way else tp < index)
                def _():
                    hop(way, index, sub).wait_send()

    for off in range(1, n_st):
        for cp in (c_cp, q_cp, t_cp, o_cp):
            cp[off].wait_send()


def local(
    tokens, pre_gain, w_gated, w_mixed, mix_weight, w_query, w_gate_mix, w_gate_read,
    store, mem_gain, w_key, w_value, passage_ids, w_out_mix, w_out_read,
):
    n_st = lax.axis_size("st")
    n_tp = lax.axis_size("tp")
    args = [
        tokens, pre_gain.reshape(1, -1), w_gated, w_mixed, mix_weight, w_query, w_gate_mix, w_gate_read,
        store, mem_gain.reshape(1, -1), w_key, w_value, passage_ids, w_out_mix, w_out_read,
    ]
    rows, model = tokens.shape
    width = w_query.shape[1]
    held, prow = store.shape[:2]
    stat_rows = max(8, 2 * (width // HD))
    take = rows // n_tp
    piece = model // SUBS
    anyspace = pl.BlockSpec(memory_space=pl.ANY)
    specs = [anyspace] * len(args)
    vm = pltpu.VMEM
    dma = pltpu.SemaphoreType.DMA
    scratch = [vm(a.shape, a.dtype) for i, a in enumerate(args) if i != 12]
    scratch += [
        vm((rows, model), BF),
        vm((n_st, rows, width), BF),
        vm((n_st, held, rows), F32),
        vm((n_st, held, rows), F32),
        vm((held * prow, width), BF),
        vm((width, held * prow), BF),
        vm((held * prow, rows), F32),
        vm((held * prow, rows), BF),
        vm((n_st, width, rows), BF),
        vm((n_st, width, rows), BF),
        vm((n_st, stat_rows, rows), F32),
        vm((n_st, stat_rows, rows), F32),
        vm((rows, w_gated.shape[1]), BF),
        vm((rows, width), BF),
        vm((2, n_tp, SUBS, take, piece), BF),
        vm((2, n_tp, SUBS, take, piece), BF),
        vm((take, model), F32),
        pltpu.SMEM(passage_ids.shape, passage_ids.dtype),
        dma((24,)),
    ]
    scratch += [dma((n_st,))] * 8 + [dma((2, n_tp, SUBS))] * 2
    return pl.pallas_call(
        functools.partial(kernel, n_st, n_tp),
        out_shape=jax.ShapeDtypeStruct((take, model), BF),
        in_specs=specs,
        out_specs=pl.BlockSpec(memory_space=pltpu.VMEM),
        scratch_shapes=scratch,
        compiler_params=pltpu.CompilerParams(
            collective_id=0, has_side_effects=True, vmem_limit_bytes=60 * 1024 * 1024
        ),
    )(*args)


def solution(mesh):
    placed = (
        P(("grp", "st"), None),
        P(),
        P(None, "tp"),
        P(None, "tp"),
        P("tp", None, None),
        P(None, "tp"),
        P(None, "tp"),
        P(None, "tp"),
        P(("grp", "st"), None, None),
        P(),
        P(None, "tp"),
        P(None, "tp"),
        P(("grp", "st"), None),
        P("tp", None),
        P("tp", None),
    )
    return jax.shard_map(
        local, mesh=mesh, in_specs=placed, out_specs=P(("grp", "st", "tp"), None), check_vma=False
    )
```

```python
import functools

import jax
import jax.numpy as jnp
from jax import lax
from jax.experimental import pallas as pl
from jax.experimental.pallas import tpu as pltpu
from jax.sharding import PartitionSpec as P

HD = 128
SPAN = 128
RBLOCK = 64
EPS = 1e-06
LOG2E = 1.4426950408889634
SUBS = 2
BF = jnp.bfloat16
F32 = jnp.float32
MESH = pl.DeviceIdType.MESH


def rms_rows(rows, gain):
    wide = rows.astype(F32)
    return (wide * lax.rsqrt(jnp.mean(wide * wide, axis=-1, keepdims=True) + EPS) * gain).astype(BF)


def silu(v):
    return v / (1.0 + jnp.exp(-v))


def dot(a, b):
    return jnp.dot(a, b, preferred_element_type=F32)


def pair_of(index, off, count):
    if count & (count - 1):
        return lax.rem(off - index + count, count)
    out, bit = 0, 1
    while bit < count:
        out = out + lax.rem(index // bit + off // bit, 2) * bit
        bit *= 2
    return out


def kernel(
    n_st, n_tp,
    tok_h, pg_h, wga_h, wmi_h, mw_h, wq_h, wgm_h, wgr_h, sto_h, mg_h, wk_h, wv_h, pid_h, wom_h, wor_h,
    out_ref,
    tok, pg, wga, wmi, mw, wq, wgm, wgr, sto, mg, wk, wv, wom, wor,
    normed, q_buf, c_send, c_buf, k_s, vt_s, s_s, p_s, o_send, o_buf, t_send, t_buf,
    om, orr, r_send, r_buf, own, pid,
    in_sem, q_ss, q_rs, c_ss, c_rs, o_ss, o_rs, t_ss, t_rs, r_ss, r_rs,
):
    st = lax.axis_index("st")
    tp = lax.axis_index("tp")
    rows = tok.shape[0]
    held = sto.shape[0]
    prow = sto.shape[1]
    width = wq.shape[1]
    heads = width // HD
    groups = mw.shape[0]
    gw = wmi.shape[1] // groups
    scale = (HD ** -0.5) * LOG2E

    pieces = 4 if held % 4 == 0 else 1
    per = held // pieces
    loads = {}
    order = [("pid", pid_h, pid), ("tok", tok_h, tok), ("pg", pg_h, pg), ("wq", wq_h, wq), ("mg", mg_h, mg),
             ("wk", wk_h, wk), ("wv", wv_h, wv)]
    late = [("wmi", wmi_h, wmi), ("wga", wga_h, wga), ("wgm", wgm_h, wgm), ("wgr", wgr_h, wgr),
            ("mw", mw_h, mw), ("wom", wom_h, wom), ("wor", wor_h, wor)]
    for i, (name, src, dst) in enumerate(order):
        loads[name] = pltpu.make_async_copy(src, dst, in_sem.at[i])
        loads[name].start()
    base = len(order)

    def store_copy(i):
        return pltpu.make_async_copy(
            sto_h.at[pl.ds(i * per, per)], sto.at[pl.ds(i * per, per)], in_sem.at[base + i]
        )

    for i in range(pieces):
        store_copy(i).start()
    for i, (name, src, dst) in enumerate(late):
        loads[name] = pltpu.make_async_copy(src, dst, in_sem.at[base + pieces + i])
        loads[name].start()

    barrier = pltpu.get_barrier_semaphore()
    for off in range(1, n_st):
        pl.semaphore_signal(barrier, inc=1, device_id={"st": pair_of(st, off, n_st)}, device_id_type=MESH)
    right = lax.rem(tp + 1, n_tp)
    left = lax.rem(tp + n_tp - 1, n_tp)
    for side in (left, right):
        pl.semaphore_signal(barrier, inc=1, device_id={"tp": side}, device_id_type=MESH)

    served = list(range(2, n_st)) + [1]
    loads["tok"].wait()
    loads["pg"].wait()
    chunk = 64
    gain = pg[...]

    def norm_step(i, carry):
        at = pl.ds(pl.multiple_of(i * chunk, chunk), chunk)
        normed[at, :] = rms_rows(tok[at, :], gain)
        return carry

    lax.fori_loop(0, rows // chunk, norm_step, 0)
    loads["pid"].wait()
    lane_block = lax.broadcasted_iota(jnp.int32, (held, rows), 1) // RBLOCK
    row_id = lax.broadcasted_iota(jnp.int32, (held, rows), 0)
    for off in range(n_st):
        mine = row_id + (pair_of(st, off, n_st) if off else st) * held
        count = jnp.zeros((held, rows), F32)
        for b in range(pid.shape[0]):
            hit = jnp.zeros((held, rows), F32)
            for n in range(pid.shape[1]):
                hit = hit + jnp.where(mine == pid[b, n], 1.0, 0.0)
            count = count + jnp.where(lane_block == b, hit, 0.0)
        c_send[off] = count
    loads["wq"].wait()
    q_buf[0] = dot(normed[...], wq[...]).astype(BF)

    pl.semaphore_wait(barrier, n_st + 1)

    def remote(src, dst, ss, rs, axis, to):
        return pltpu.make_async_remote_copy(
            src_ref=src, dst_ref=dst, send_sem=ss, recv_sem=rs, device_id={axis: to}, device_id_type=MESH
        )

    q_cp, c_cp, o_cp, t_cp = {}, {}, {}, {}
    near = pair_of(st, 1, n_st)
    for off in served:
        to = pair_of(st, off, n_st)
        c_cp[off] = remote(c_send.at[off], c_buf.at[off], c_ss.at[off], c_rs.at[off], "st", to)
        c_cp[off].start()
    for off in served:
        if off % 2 and off > 1:
            q_cp[off] = remote(q_buf.at[off - 1], q_buf.at[off], q_ss.at[off], q_rs.at[off], "st", near)
        else:
            q_cp[off] = remote(
                q_buf.at[0], q_buf.at[off], q_ss.at[off], q_rs.at[off], "st", pair_of(st, off, n_st)
            )
            q_cp[off].start()
    c_buf[0] = c_send[0]

    loads["mg"].wait()
    loads["wk"].wait()
    loads["wv"].wait()
    mgain = mg[...]
    span = per * prow

    def kv_step(i, carry):
        store_copy(i).wait()
        part = sto[pl.ds(i * per, per)].reshape(span, sto.shape[2])
        rows_n = rms_rows(part, mgain)
        at = pl.ds(pl.multiple_of(i * span, span), span)
        k_s[at, :] = dot(rows_n, wk[...]).astype(BF)
        vt_s[:, at] = dot(rows_n, wv[...]).T.astype(BF)
        return carry

    lax.fori_loop(0, pieces, kv_step, 0)

    loads["wmi"].wait()
    mixed = dot(normed[...], wmi[...])
    for off in range(2, n_st - 1, 2):
        q_cp[off].wait_recv()
        q_cp[off + 1].start()
    gid = lax.broadcasted_iota(jnp.int32, (1, mixed.shape[1]), 1) // gw
    centre = mixed
    for g in range(groups):
        mean = jnp.sum(jnp.where(gid == g, mixed, 0.0), axis=-1, keepdims=True) * (1.0 / gw)
        centre = jnp.where(gid == g, mixed - mean, centre)
    square = centre * centre
    factor = jnp.zeros_like(mixed)
    for g in range(groups):
        var = jnp.sum(jnp.where(gid == g, square, 0.0), axis=-1, keepdims=True) * (1.0 / gw)
        factor = jnp.where(gid == g, lax.rsqrt(var + EPS), factor)
    mixed_norm = (centre * factor).astype(BF)

    def attend(off):
        reader_counts = c_buf[off]
        stats = []
        for h in range(heads):
            cols = slice(h * HD, (h + 1) * HD)
            s_s[...] = lax.dot_general(
                k_s[:, cols], q_buf[off, :, cols], (((1,), (1,)), ((), ())), preferred_element_type=F32
            )
            top = jnp.full((1, rows), -1e30, F32)
            for j in range(held):
                one = jnp.max(s_s[j * prow:(j + 1) * prow, :], axis=0, keepdims=True)
                top = jnp.where(reader_counts[j:j + 1, :] > 0.0, jnp.maximum(top, one), top)
            total = jnp.zeros((1, rows), F32)
            for j in range(held):
                at = slice(j * prow, (j + 1) * prow)
                times = reader_counts[j:j + 1, :]
                off_by = jnp.where(times > 0.0, top, 1e30)
                e = jnp.exp2((s_s[at, :] - off_by) * scale) * times
                total = total + jnp.sum(e, axis=0, keepdims=True)
                p_s[at, :] = e.astype(BF)
            inverse = jnp.where(total > 0.0, 1.0 / jnp.where(total > 0.0, total, 1.0), 0.0)
            read = dot(vt_s[cols, :], p_s[...]) * inverse
            if off == 0:
                o_buf[0, cols, :] = read.astype(BF)
            else:
                o_send[off, cols, :] = read.astype(BF)
            stats += [top, total]
        pad = t_send.shape[1] - len(stats)
        if pad:
            stats.append(jnp.zeros((pad, rows), F32))
        if off == 0:
            t_buf[0] = jnp.concatenate(stats, axis=0)
        else:
            t_send[off] = jnp.concatenate(stats, axis=0)

    for off in served:
        if off % 2 or off == n_st - 1:
            q_cp[off].wait_recv()
        c_cp[off].wait_recv()
        attend(off)
        to = pair_of(st, off, n_st)
        t_cp[off] = remote(t_send.at[off], t_buf.at[off], t_ss.at[off], t_rs.at[off], "st", to)
        o_cp[off] = remote(o_send.at[off], o_buf.at[off], o_ss.at[off], o_rs.at[off], "st", to)
        t_cp[off].start()
        o_cp[off].start()
    attend(0)

    loads["mw"].wait()
    lower = lax.broadcasted_iota(jnp.int32, (SPAN, SPAN), 1) <= lax.broadcasted_iota(jnp.int32, (SPAN, SPAN), 0)
    weights = [jnp.where(lower, mw[g].astype(F32), 0.0).astype(BF) for g in range(groups)]
    parts = []
    for n in range(rows // SPAN):
        block = mixed_norm[n * SPAN:(n + 1) * SPAN, :]
        spatial = dot(weights[0], block)
        for g in range(1, groups):
            spatial = jnp.where(gid == g, dot(weights[g], block), spatial)
        parts.append(spatial)
    spatial = jnp.concatenate(parts, axis=0)
    loads["wga"].wait()
    branch = dot(normed[...], wga[...]) * spatial
    loads["wgm"].wait()
    om[...] = (branch * silu(dot(normed[...], wgm[...]))).astype(BF)
    loads["wgr"].wait()
    gate_read = silu(dot(normed[...], wgr[...]))

    for off in range(1, n_st):
        t_cp[off].wait_recv()
        o_cp[off].wait_recv()
    for h in range(heads):
        cols = slice(h * HD, (h + 1) * HD)
        tops = [t_buf[i, 2 * h:2 * h + 1, :] for i in range(n_st)]
        top = functools.reduce(jnp.maximum, tops)
        shares = [jnp.exp2((tops[i] - top) * scale) * t_buf[i, 2 * h + 1:2 * h + 2, :] for i in range(n_st)]
        inverse = 1.0 / functools.reduce(jnp.add, shares)
        read = jnp.zeros((HD, rows), F32)
        for i in range(n_st):
            read = read + o_buf[i, cols, :].astype(F32) * (shares[i] * inverse)
        orr[:, cols] = (read.T * gate_read[:, cols]).astype(BF)

    loads["wom"].wait()
    loads["wor"].wait()
    take = rows // n_tp
    piece = wom.shape[1] // SUBS

    def partial(index, chain):
        at = pl.ds(pl.multiple_of(index * take, take), take)
        cols = pl.ds(pl.multiple_of(chain * piece, 128), piece)
        return dot(om[at, :], wom[:, cols]) + dot(orr[at, :], wor[:, cols])

    def hop(way, index, sub):
        return remote(
            r_send.at[way, index, sub], r_buf.at[way, index, sub],
            r_ss.at[way, index, sub], r_rs.at[way, index, sub],
            "tp", left if way else right,
        )

    def ring_step(t, carry):
        for way in range(2):
            place = t - (n_tp - 1 - tp if way else tp)
            sub = lax.rem(place + n_tp * SUBS, SUBS)
            turn = (place + n_tp * SUBS) // SUBS - n_tp
            index = turn if way else n_tp - 1 - turn
            sends = (index < tp) if way else (index > tp)
            takes = tp < n_tp - 1 if way else tp > 0

            @pl.when((place >= 0) & (place < (n_tp - 1) * SUBS) & sends)
            def _():
                value = partial(index, sub)

                @pl.when(takes)
                def _():
                    hop(way, index, sub).wait_recv()
                    r_send[way, index, sub] = (value + r_buf[way, index, sub].astype(F32)).astype(BF)

                @pl.when(jnp.logical_not(takes))
                def _():
                    r_send[way, index, sub] = value.astype(BF)

                hop(way, index, sub).start()

        return carry

    lax.fori_loop(0, (n_tp - 1) * SUBS + n_tp - 1, ring_step, 0)

    for sub in range(SUBS):
        own[:, sub * piece:(sub + 1) * piece] = partial(tp, sub)
    for index in range(n_tp):
        @pl.when(tp == index)
        def _():
            for sub in range(SUBS):
                value = own[:, sub * piece:(sub + 1) * piece]
                if index < n_tp - 1:
                    hop(1, index, sub).wait_recv()
                    value = value + r_buf[1, index, sub].astype(F32)
                if index > 0:
                    hop(0, index, sub).wait_recv()
                    value = value + r_buf[0, index, sub].astype(F32)
                out_ref[:, sub * piece:(sub + 1) * piece] = value.astype(BF)

    for k in range(n_tp - 1):
        for sub in range(SUBS):
            for way, index in ((0, n_tp - 1 - k), (1, k)):
                @pl.when(tp > index if way else tp < index)
                def _():
                    hop(way, index, sub).wait_send()

    for off in range(1, n_st):
        for cp in (c_cp, q_cp, t_cp, o_cp):
            cp[off].wait_send()


def local(
    tokens, pre_gain, w_gated, w_mixed, mix_weight, w_query, w_gate_mix, w_gate_read,
    store, mem_gain, w_key, w_value, passage_ids, w_out_mix, w_out_read,
):
    n_st = lax.axis_size("st")
    n_tp = lax.axis_size("tp")
    args = [
        tokens, pre_gain.reshape(1, -1), w_gated, w_mixed, mix_weight, w_query, w_gate_mix, w_gate_read,
        store, mem_gain.reshape(1, -1), w_key, w_value, passage_ids, w_out_mix, w_out_read,
    ]
    rows, model = tokens.shape
    width = w_query.shape[1]
    held, prow = store.shape[:2]
    stat_rows = max(8, 2 * (width // HD))
    take = rows // n_tp
    piece = model // SUBS
    anyspace = pl.BlockSpec(memory_space=pl.ANY)
    specs = [anyspace] * len(args)
    vm = pltpu.VMEM
    dma = pltpu.SemaphoreType.DMA
    scratch = [vm(a.shape, a.dtype) for i, a in enumerate(args) if i != 12]
    scratch += [
        vm((rows, model), BF),
        vm((n_st, rows, width), BF),
        vm((n_st, held, rows), F32),
        vm((n_st, held, rows), F32),
        vm((held * prow, width), BF),
        vm((width, held * prow), BF),
        vm((held * prow, rows), F32),
        vm((held * prow, rows), BF),
        vm((n_st, width, rows), BF),
        vm((n_st, width, rows), BF),
        vm((n_st, stat_rows, rows), F32),
        vm((n_st, stat_rows, rows), F32),
        vm((rows, w_gated.shape[1]), BF),
        vm((rows, width), BF),
        vm((2, n_tp, SUBS, take, piece), BF),
        vm((2, n_tp, SUBS, take, piece), BF),
        vm((take, model), F32),
        pltpu.SMEM(passage_ids.shape, passage_ids.dtype),
        dma((24,)),
    ]
    scratch += [dma((n_st,))] * 8 + [dma((2, n_tp, SUBS))] * 2
    return pl.pallas_call(
        functools.partial(kernel, n_st, n_tp),
        out_shape=jax.ShapeDtypeStruct((take, model), BF),
        in_specs=specs,
        out_specs=pl.BlockSpec(memory_space=pltpu.VMEM),
        scratch_shapes=scratch,
        compiler_params=pltpu.CompilerParams(
            collective_id=0, has_side_effects=True, vmem_limit_bytes=60 * 1024 * 1024
        ),
    )(*args)


def solution(mesh):
    placed = (
        P(("grp", "st"), None),
        P(),
        P(None, "tp"),
        P(None, "tp"),
        P("tp", None, None),
        P(None, "tp"),
        P(None, "tp"),
        P(None, "tp"),
        P(("grp", "st"), None, None),
        P(),
        P(None, "tp"),
        P(None, "tp"),
        P(("grp", "st"), None),
        P("tp", None),
        P("tp", None),
    )
    return jax.shard_map(
        local, mesh=mesh, in_specs=placed, out_specs=P(("grp", "st", "tp"), None), check_vma=False
    )
```
